32 devices in a mesh: fs: 8 (over z, x), tp: 4 (over y, core).
Axes of the slice: x: 2, y: 2, z: 4, core: 2. Of those that a mesh axis runs over, the one named last changes fastest.
Arguments:
- saved_input: bfloat16 [20480, 2048], P('fs'), may hold values from -6 to 6
- value_cot: bfloat16 [20480, 1024], P('fs', 'tp'), may hold values from -6 to 6
- query_cot: bfloat16 [20480, 512], P('fs', 'tp'), may hold values from -6 to 6
- value_master: float32 [2048, 1024], P('fs', 'tp'), may hold values from -0.125 to 0.125
- query_master: float32 [2048, 512], P('fs', 'tp'), may hold values from -0.125 to 0.125
- value_factor: bfloat16 [2048, 256], P('fs'), may hold values from -0.125 to 0.125
- query_factor: bfloat16 [2048, 256], P('fs'), may hold values from -0.125 to 0.125
- value_first: float32 [256, 1024], P('fs', 'tp'), as said below
- value_second: float32 [256, 1024], P('fs', 'tp'), as said below
- query_first: float32 [256, 512], P('fs', 'tp'), as said below
- query_second: float32 [256, 512], P('fs', 'tp'), as said below
Outputs:
- value_step: float32 [2048, 1024], P('fs', 'tp')
- query_step: float32 [2048, 512], P('fs', 'tp')
- value_master_new: float32 [2048, 1024], P('fs', 'tp')
- query_master_new: float32 [2048, 512], P('fs', 'tp')
- value_copy: bfloat16 [2048, 1024], P(None, 'tp')
- query_copy: bfloat16 [2048, 512], P(None, 'tp')
- value_first_new: float32 [256, 1024], P('fs', 'tp')
- value_second_new: float32 [256, 1024], P('fs', 'tp')
- query_first_new: float32 [256, 512], P('fs', 'tp')
- query_second_new: float32 [256, 512], P('fs', 'tp')
The draws below stay inside these ranges and needn't reach their ends.
Inputs may be any that keep to these rules, and one draw needn't show every extreme that they name: `value_first`: first moments are real-valued of the projected gradient's order. `value_second`: second moments are positive. `query_first`: first moments are real-valued of the projected gradient's order. `query_second`: second moments are positive.
All inputs are finite; a program needn't handle non-finite values.
Results may differ from the reference program's by a relative error of at most 0.001.
Values may be sent and summed in bfloat16 or wider, within the bound.
A program may use at most 64 MiB of HBM per device.

```python
import jax
import jax.numpy as jnp
from jax import lax

D = 2048
RANK = 256
TOKENS = 20480
V_W = 1024
QK_W = 512


def first_draw(key, width):
    level = 0.1 / jnp.sqrt(jnp.float32(TOKENS))
    values = jax.random.normal(jax.random.fold_in(key, 11), (RANK, width), jnp.float32)
    return values * level


def second_draw(key, width):
    level = 0.05 / jnp.float32(TOKENS)
    row_pos = jnp.arange(RANK, dtype=jnp.float32)[:, None] / RANK
    col_pos = jnp.arange(width, dtype=jnp.float32)[None, :] / width
    spread = jnp.exp(jax.random.uniform(jax.random.fold_in(key, 13), (RANK, width), jnp.float32, -0.7, 0.7))
    rising = 10.0 ** row_pos * 10.0 ** col_pos
    return level * spread * rising


def draw_value_first(key, part):
    return first_draw(key, V_W)


def draw_value_second(key, part):
    return second_draw(key, V_W)


def draw_query_first(key, part):
    return first_draw(key, QK_W)


def draw_query_second(key, part):
    return second_draw(key, QK_W)


def strengthened(entries, own_key, source, target, shards_of, factor):
    owner, partner = [(jnp.arange(entries.shape[axis_at]) // (entries.shape[axis_at] // shards_of)).reshape([-1 if axis == axis_at else 1 for axis in range(entries.ndim)]) for axis_at in (source, target)]
    chosen = jax.random.permutation(own_key, shards_of)[partner]
    strong = (owner == chosen) | (owner == (partner + shards_of // 2) % shards_of)
    return jnp.where(strong, factor * entries, entries)


def steps_of(stream_key, dims, pieces, smallest, top_value):
    factor_of, own = 1.0, jax.random.fold_in(stream_key, 6)
    for position, shards_of in pieces:
        draws = jnp.exp(jax.random.uniform(jax.random.fold_in(own, position), (shards_of,), jnp.float32, smallest / len(pieces), top_value / len(pieces)))
        factor_of = factor_of * jnp.repeat(draws, dims[position] // shards_of).reshape([-1 if axis == position else 1 for axis in range(len(dims))])
    return factor_of


def noise(key, dims, scale, bound, cuts=(), held_as=jnp.bfloat16):
    values = scale * jax.random.normal(key, dims, jnp.float32)
    if cuts:
        values = values * steps_of(key, dims, cuts, -0.22, 0.18)
    return jnp.clip(values, -bound, bound).astype(held_as)


def heavy_noise(rng, dims, scale, bound, shards, heavy, kind=jnp.bfloat16):
    values = scale * jax.random.normal(rng, dims, jnp.float32)
    if shards:
        values = values * steps_of(rng, dims, shards, -0.22, 0.18)
    return jnp.clip(strengthened(values, jax.random.fold_in(rng, 3), *heavy), -bound, bound).astype(kind)


def setup_inputs(seed: int = 0) -> dict:
    arg_keys = jax.random.split(jax.random.key(seed), 12)
    return {
        "saved_input": heavy_noise(arg_keys[0], (TOKENS, D), 1.0, 6.0, ((0, 8),), (0, 1, 8, 2.0)),
        "value_cot": noise(arg_keys[1], (TOKENS, V_W), 1.0, 6.0, ((0, 8), (1, 4))),
        "query_cot": noise(arg_keys[2], (TOKENS, QK_W), 1.0, 6.0, ((0, 8), (1, 4))),
        "value_master": noise(arg_keys[3], (D, V_W), D ** -0.5, 0.125, ((0, 8), (1, 4)), jnp.float32),
        "query_master": noise(arg_keys[4], (D, QK_W), D ** -0.5, 0.125, ((0, 8), (1, 4)), jnp.float32),
        "value_factor": noise(arg_keys[5], (D, RANK), D ** -0.5, 0.125, ((0, 8),)),
        "query_factor": noise(arg_keys[6], (D, RANK), D ** -0.5, 0.125, ((0, 8),)),
        "value_first": draw_value_first(jax.random.fold_in(arg_keys[11], 71), 0),
        "value_second": draw_value_second(jax.random.fold_in(arg_keys[11], 71), 0),
        "query_first": draw_query_first(jax.random.fold_in(arg_keys[11], 71), 0),
        "query_second": draw_query_second(jax.random.fold_in(arg_keys[11], 71), 0),
    }


BETA_ONE = 0.9
BETA_TWO = 0.95
DENOM_EPS = 1e-08
NORM_EPS = 1e-06
STEP_SIZE = 0.05

def moment_update(factor, gradient, first, second):
    projected = jnp.dot(factor.astype(jnp.float32).T, gradient, precision=lax.Precision.HIGHEST)
    first_new = BETA_ONE * first + (1.0 - BETA_ONE) * projected
    second_new = BETA_TWO * second + (1.0 - BETA_TWO) * projected * projected
    direction = first_new / (jnp.sqrt(second_new) + DENOM_EPS)
    return (first_new, second_new, direction)

def reference(saved_input, value_cot, query_cot, value_master, query_master, value_factor, query_factor, value_first, value_second, query_first, query_second):
    value_grad = jnp.dot(saved_input.T, value_cot, preferred_element_type=jnp.float32) / TOKENS
    query_grad = jnp.dot(saved_input.T, query_cot, preferred_element_type=jnp.float32) / TOKENS
    value_first_new, value_second_new, value_direction = moment_update(value_factor, value_grad, value_first, value_second)
    query_first_new, query_second_new, query_direction = moment_update(query_factor, query_grad, query_first, query_second)
    square_sum = jnp.sum(value_direction * value_direction) + jnp.sum(query_direction * query_direction)
    update_scale = 1.0 / jnp.sqrt(square_sum / (RANK * (V_W + QK_W)) + NORM_EPS)
    value_step = jnp.dot(value_factor.astype(jnp.float32), value_direction, precision=lax.Precision.HIGHEST) * update_scale
    query_step = jnp.dot(query_factor.astype(jnp.float32), query_direction, precision=lax.Precision.HIGHEST) * update_scale
    value_master_new = value_master - STEP_SIZE * value_step
    query_master_new = query_master - STEP_SIZE * query_step
    return (value_step, query_step, value_master_new, query_master_new, value_master_new.astype(jnp.bfloat16), query_master_new.astype(jnp.bfloat16), value_first_new, value_second_new, query_first_new, query_second_new)
```

```python
import functools

import jax
import jax.numpy as jnp
from jax import lax
from jax.experimental import pallas as pl
from jax.experimental.pallas import tpu as pltpu
from jax.sharding import PartitionSpec as P

BETA_ONE = 0.9
BETA_TWO = 0.95
DENOM_EPS = 1e-08
NORM_EPS = 1e-06
STEP_SIZE = 0.05

MESH = pl.DeviceIdType.MESH
F32 = jnp.float32
BF16 = jnp.bfloat16


def split_dot(lhs, rhs):
    return jnp.dot(lhs, rhs, preferred_element_type=F32)


class Gather:
    def __init__(self, slot, parts, nz, nx, me, send_sem, recv_sem, extra=None):
        self.slot, self.parts, self.nz, self.nx = slot, parts, nz, nx
        self.me, self.z, self.x = me, me // nx, me % nx
        self.send_sem, self.recv_sem, self.extra = send_sem, recv_sem, extra
        self.sent = []

    def copy(self, part, index, kind, peer):
        ref = self.slot(index, part)
        return pltpu.make_async_remote_copy(
            src_ref=ref,
            dst_ref=ref,
            send_sem=self.send_sem.at[part, index, kind],
            recv_sem=self.recv_sem.at[part, index],
            device_id={"fs": peer},
            device_id_type=MESH,
        )

    def send(self, part, index, kind, peer, where):
        def go():
            self.copy(part, index, kind, peer).start()

        def done():
            self.copy(part, index, kind, peer).wait_send()

        pl.when(where)(go)
        self.sent.append((where, done))

    def up(self, part, index, where):
        self.send(part, index, 0, jnp.minimum(self.me + self.nx, self.nz * self.nx - 1),
                  jnp.logical_and(where, self.z < self.nz - 1))

    def down(self, part, index, where):
        self.send(part, index, 1, jnp.maximum(self.me - self.nx, 0), jnp.logical_and(where, self.z > 0))

    def across(self, part, index, where):
        for k in range(1, self.nx):
            peer = self.z * self.nx + (self.x + k) % self.nx
            self.send(part, index, 1 + k, peer, where)

    def arrived(self, part, index, where):
        def go():
            self.copy(part, index, 0, self.me).wait_recv()
            if self.extra is not None:
                self.extra(part, index)

        pl.when(where)(go)

    def start(self):
        yes = self.z >= 0
        for part in range(self.parts):
            if part == 1:
                self.across(part, self.me, yes)
            self.up(part, self.me, yes)
            self.down(part, self.me, yes)
            if part == 0:
                self.across(part, self.me, yes)

    def side(self):
        yes = self.z >= 0
        for k in range(1, self.nx):
            index = self.z * self.nx + (self.x + k) % self.nx
            if self.parts > 1:
                self.arrived(1, index, yes)
                self.up(1, index, yes)
                self.down(1, index, yes)

    def hop(self, s):
        below, above = self.z >= s, self.z + s < self.nz
        low = jnp.maximum(self.z - s, 0) * self.nx
        high = jnp.minimum(self.z + s, self.nz - 1) * self.nx
        for where, base, onward in ((below, low, self.up), (above, high, self.down)):
            index = base + self.x
            self.arrived(0, index, where)
            onward(0, index, where)
            self.across(0, index, where)
            if self.parts > 1:
                for k in range(self.nx):
                    index = base + (self.x + k) % self.nx
                    self.arrived(1, index, where)
                    onward(1, index, where)

    def last(self):
        yes = self.z >= 0
        for z in range(self.nz):
            for k in range(1, self.nx):
                self.arrived(0, z * self.nx + (self.x + k) % self.nx, yes)

    def drain(self):
        for where, done in self.sent:
            pl.when(where)(done)

    def whole(self):
        self.start()
        self.side()
        for s in range(1, self.nz):
            self.hop(s)
        self.last()


def kernel(
    nfs, ntp, nz, nx, total_tokens, entries,
    x_in, cv_in, cq_in, mv_in, mq_in, fv_in, fq_in, v1_in, v2_in, q1_in, q2_in,
    step_v, step_q, new_v, new_q, copy_v, copy_q, v1, v2, q1, q2,
    xs, cv, cq, ct, gh, gl, fac, part, landed, dirs, sums, cop, mv, mq, m1v, m2v, m1q, m2q,
    load_sem, x_sem, fsend, frecv, sib_send, sib_recv, dsend, drecv, csend, crecv, rs_sem, sum_sem,
):
    me, tp = lax.axis_index("fs"), lax.axis_index("tp")
    core, sibling = tp % 2, tp + 1 - 2 * (tp % 2)
    blocks, tokens, width = xs.shape
    rows, rank = fv_in.shape
    wv, wq = cv.shape[1], cq.shape[1]
    rk = v1_in.shape[0]
    fparts, fhalf = fac.shape[2], fac.shape[3]
    dparts, dhalf = dirs.shape[1], dirs.shape[2]
    cparts, chalf = cop.shape[1], cop.shape[2]

    loads = []

    def load(src, dst):
        copy = pltpu.make_async_copy(src, dst, load_sem.at[len(loads)])
        copy.start()
        loads.append(copy)

    for p in range(fparts):
        load(fv_in.at[pl.ds(p * fhalf, fhalf)], fac.at[0, me, p])
        load(fq_in.at[pl.ds(p * fhalf, fhalf)], fac.at[1, me, p])
    nfac = len(loads)
    load(cv_in, cv)
    load(cq_in, cq)
    xcopies = []
    for b in range(blocks):
        copy = pltpu.make_async_copy(x_in.at[:, pl.ds(b * width, width)], xs.at[b], x_sem.at[b])
        copy.start()
        xcopies.append(copy)
    for src, dst in ((v1_in, m1v), (v2_in, m2v), (q1_in, m1q), (q2_in, m2q), (mv_in, mv), (mq_in, mq)):
        load(src, dst)

    barrier = pltpu.get_barrier_semaphore()
    devices = nfs * ntp
    mine = me * ntp + tp

    def greet(k, _):
        other = (mine + k) % devices
        pl.semaphore_signal(
            barrier, inc=1, device_id={"fs": other // ntp, "tp": other % ntp}, device_id_type=MESH
        )
        return 0

    lax.fori_loop(1, devices, greet, 0)
    for copy in loads[:nfac]:
        copy.wait()
    pl.semaphore_wait(barrier, devices - 1)

    def to_sibling(p, index):
        return pltpu.make_async_remote_copy(
            src_ref=fac.at[core, index, p],
            dst_ref=fac.at[core, index, p],
            send_sem=sib_send.at[p, index],
            recv_sem=sib_recv.at[p, index],
            device_id={"tp": sibling},
            device_id_type=MESH,
        )

    factors = Gather(
        lambda index, p: fac.at[core, index, p], fparts, nz, nx, me, fsend, frecv,
        extra=lambda p, index: to_sibling(p, index).start(),
    )
    factors.start()

    loads[nfac].wait()
    loads[nfac + 1].wait()
    ct[0:wv, :] = cv[...].T
    ct[wv : wv + wq, :] = cq[...].T
    inverse = 1.0 / total_tokens

    def grad_block(b):
        xcopies[b].wait()
        g = split_dot(ct[...], xs[b]) * inverse
        high = g.astype(BF16)
        gh[b] = high
        gl[b] = (g - high.astype(F32)).astype(BF16)

    todo = [factors.side] + [functools.partial(factors.hop, s) for s in range(1, nz)]
    for b in range(blocks):
        grad_block(b)
        if b < len(todo):
            todo[b]()
    for work in todo[blocks:]:
        work()
    factors.last()
    for p in range(fparts):
        for k in range(1, nfs):
            index = (me + k) % nfs
            pltpu.make_async_remote_copy(
                src_ref=fac.at[1 - core, index, p],
                dst_ref=fac.at[1 - core, index, p],
                send_sem=sib_send.at[p, index],
                recv_sem=sib_recv.at[p, index],
                device_id={"tp": sibling},
                device_id_type=MESH,
            ).wait_recv()

    all_v = fac[0].reshape(blocks, width, rank)
    all_q = fac[1].reshape(blocks, width, rank)
    acc_v = jnp.zeros((wv, rank), F32)
    acc_q = jnp.zeros((wq, rank), F32)
    for b in range(blocks):
        for g in (gl, gh):
            acc_v += split_dot(g[b, 0:wv, :], all_v[b])
            acc_q += split_dot(g[b, wv : wv + wq, :], all_q[b])
    part[:, :, 0:wv] = acc_v.T.reshape(nfs, rk, wv)
    part[:, :, wv : wv + wq] = acc_q.T.reshape(nfs, rk, wq)

    for k in range(1, nfs):
        peer = (me + k) % nfs
        pltpu.make_async_remote_copy(
            src_ref=part.at[peer],
            dst_ref=landed.at[k - 1],
            send_sem=rs_sem.at[0],
            recv_sem=rs_sem.at[1],
            device_id={"fs": peer},
            device_id_type=MESH,
        ).start()
    for copy in loads[nfac + 2 :]:
        copy.wait()
    everything = pltpu.make_async_remote_copy(
        src_ref=landed,
        dst_ref=landed,
        send_sem=rs_sem.at[0],
        recv_sem=rs_sem.at[1],
        device_id={"fs": me},
        device_id_type=MESH,
    )
    everything.wait_recv()
    share = part[me]
    for k in range(nfs - 1):
        share = share + landed[k]

    square = jnp.zeros((), F32)
    for cols, first_ref, second_ref, first_out, second_out in (
        (slice(0, wv), m1v, m2v, v1, v2),
        (slice(wv, wv + wq), m1q, m2q, q1, q2),
    ):
        projected = share[:, cols]
        first_new = BETA_ONE * first_ref[...] + (1.0 - BETA_ONE) * projected
        second_new = BETA_TWO * second_ref[...] + (1.0 - BETA_TWO) * projected * projected
        first_out[...] = first_new
        second_out[...] = second_new
        direction = first_new / (jnp.sqrt(second_new) + DENOM_EPS)
        dirs[me, :, :, cols] = direction.reshape(dparts, dhalf, direction.shape[1])
        square = square + jnp.sum(direction * direction)
    sums[devices - 1] = jnp.full(sums.shape[1:], square, F32)

    directions = Gather(lambda index, p: dirs.at[index, p], dparts, nz, nx, me, dsend, drecv)
    directions.start()

    def tell(k, _):
        other = (mine + k) % devices
        pltpu.make_async_remote_copy(
            src_ref=sums.at[devices - 1],
            dst_ref=sums.at[devices - 1 - k],
            send_sem=sum_sem.at[0],
            recv_sem=sum_sem.at[1],
            device_id={"fs": other // ntp, "tp": other % ntp},
            device_id_type=MESH,
        ).start()
        return 0

    lax.fori_loop(1, devices, tell, 0)
    directions.side()
    for s in range(1, nz):
        directions.hop(s)
    directions.last()

    full = dirs[...].reshape(rank, wv + wq)
    high = full.astype(BF16)
    low = (full - high.astype(F32)).astype(BF16)
    own_v = fac[0, me].reshape(rows, rank)
    own_q = fac[1, me].reshape(rows, rank)
    raw_v = split_dot(own_v, low[:, 0:wv]) + split_dot(own_v, high[:, 0:wv])
    raw_q = split_dot(own_q, low[:, wv:]) + split_dot(own_q, high[:, wv:])

    told = pltpu.make_async_remote_copy(
        src_ref=sums.at[pl.ds(0, devices - 1)],
        dst_ref=sums.at[pl.ds(0, devices - 1)],
        send_sem=sum_sem.at[0],
        recv_sem=sum_sem.at[1],
        device_id={"fs": me},
        device_id_type=MESH,
    )
    told.wait_recv()
    square_sum = jnp.sum(sums[...], axis=0)[0:1, 0:1]
    scale = 1.0 / jnp.sqrt(square_sum / entries + NORM_EPS)
    sv = raw_v * scale
    sq = raw_q * scale
    nv = mv[...] - STEP_SIZE * sv
    nq = mq[...] - STEP_SIZE * sq
    step_v[...] = sv
    step_q[...] = sq
    new_v[...] = nv
    new_q[...] = nq
    cop[me, :, :, 0:wv] = nv.astype(BF16).reshape(cparts, chalf, wv)
    cop[me, :, :, wv : wv + wq] = nq.astype(BF16).reshape(cparts, chalf, wq)
    copies = Gather(lambda index, p: cop.at[index, p], cparts, nz, nx, me, csend, crecv)
    copies.whole()
    copy_v[...] = cop[:, :, :, 0:wv].reshape(nfs * rows, wv)
    copy_q[...] = cop[:, :, :, wv : wv + wq].reshape(nfs * rows, wq)

    factors.drain()
    for p in range(fparts):
        for k in range(1, nfs):
            to_sibling(p, (me + k) % nfs).wait_send()
    everything.wait_send()
    told.wait_send()
    directions.drain()
    copies.drain()


def grid_of(n):
    nx = 1
    for d in range(1, n + 1):
        if n % d == 0 and d * d <= n:
            nx = d
    return n // nx, nx


def solution(mesh):
    nfs, ntp = mesh.shape["fs"], mesh.shape["tp"]
    nz, nx = grid_of(nfs)

    def step(x, cv, cq, mv, mq, fv, fq, v1, v2, q1, q2):
        tokens, depth = x.shape
        wv, wq = cv.shape[1], cq.shape[1]
        rows, rank = fv.shape
        rk = v1.shape[0]
        w = wv + wq
        blocks = 4
        width = depth // blocks
        two = lambda size, tile: 2 if size % (2 * tile) == 0 else 1
        fparts, dparts, cparts = two(rows, 16), two(rk, 8), two(rows, 16)
        kinds = 1 + nx
        dma = pltpu.SemaphoreType.DMA
        like = lambda shape, dtype: jax.ShapeDtypeStruct(shape, dtype)
        return pl.pallas_call(
            functools.partial(
                kernel, nfs, ntp, nz, nx, float(tokens * nfs), float(rank * w * ntp)
            ),
            out_shape=(
                like((rows, wv), F32), like((rows, wq), F32),
                like((rows, wv), F32), like((rows, wq), F32),
                like((depth, wv), BF16), like((depth, wq), BF16),
                like((rk, wv), F32), like((rk, wv), F32),
                like((rk, wq), F32), like((rk, wq), F32),
            ),
            in_specs=[pl.BlockSpec(memory_space=pl.ANY)] * 11,
            out_specs=tuple([pl.BlockSpec(memory_space=pltpu.VMEM)] * 10),
            scratch_shapes=[
                pltpu.VMEM((blocks, tokens, width), BF16),
                pltpu.VMEM((tokens, wv), BF16),
                pltpu.VMEM((tokens, wq), BF16),
                pltpu.VMEM((w, tokens), BF16),
                pltpu.VMEM((blocks, w, width), BF16),
                pltpu.VMEM((blocks, w, width), BF16),
                pltpu.VMEM((2, nfs, fparts, rows // fparts, rank), BF16),
                pltpu.VMEM((nfs, rk, w), F32),
                pltpu.VMEM((nfs - 1, rk, w), F32),
                pltpu.VMEM((nfs, dparts, rk // dparts, w), F32),
                pltpu.VMEM((nfs * ntp, 8, 128), F32),
                pltpu.VMEM((nfs, cparts, rows // cparts, w), BF16),
                pltpu.VMEM((rows, wv), F32),
                pltpu.VMEM((rows, wq), F32),
                pltpu.VMEM((rk, wv), F32),
                pltpu.VMEM((rk, wv), F32),
                pltpu.VMEM((rk, wq), F32),
                pltpu.VMEM((rk, wq), F32),
                dma((2 * fparts + 8,)),
                dma((blocks,)),
                dma((fparts, nfs, kinds)),
                dma((fparts, nfs)),
                dma((fparts, nfs)),
                dma((fparts, nfs)),
                dma((dparts, nfs, kinds)),
                dma((dparts, nfs)),
                dma((cparts, nfs, kinds)),
                dma((cparts, nfs)),
                dma((2,)),
                dma((2,)),
            ],
            compiler_params=pltpu.CompilerParams(
                collective_id=0, has_side_effects=True, vmem_limit_bytes=56 * 1024 * 1024
            ),
            name="moment_step",
        )(x, cv, cq, mv, mq, fv, fq, v1, v2, q1, q2)

    tall, both = P("fs", None), P("fs", "tp")
    return jax.shard_map(
        step,
        mesh=mesh,
        in_specs=(tall, both, both, both, both, tall, tall, both, both, both, both),
        out_specs=(both, both, both, both, P(None, "tp"), P(None, "tp"), both, both, both, both),
        check_vma=False,
    )
```

```python
import functools

import jax
import jax.numpy as jnp
from jax import lax
from jax.experimental import pallas as pl
from jax.experimental.pallas import tpu as pltpu
from jax.sharding import PartitionSpec as P

BETA_ONE = 0.9
BETA_TWO = 0.95
DENOM_EPS = 1e-08
NORM_EPS = 1e-06
STEP_SIZE = 0.05

MESH = pl.DeviceIdType.MESH
F32 = jnp.float32
BF16 = jnp.bfloat16


def split_dot(lhs, rhs):
    return jnp.dot(lhs, rhs, preferred_element_type=F32)


class Gather:
    def __init__(self, slot, parts, nz, nx, me, send_sem, recv_sem, extra=None):
        self.slot, self.parts, self.nz, self.nx = slot, parts, nz, nx
        self.me, self.z, self.x = me, me // nx, me % nx
        self.send_sem, self.recv_sem, self.extra = send_sem, recv_sem, extra
        self.sent = []
        self.direct = max(parts - 1, 1)

    def copy(self, part, index, kind, peer):
        ref = self.slot(index, part)
        return pltpu.make_async_remote_copy(
            src_ref=ref,
            dst_ref=ref,
            send_sem=self.send_sem.at[part, index, kind],
            recv_sem=self.recv_sem.at[part, index],
            device_id={"fs": peer},
            device_id_type=MESH,
        )

    def send(self, part, index, kind, peer, where):
        def go():
            self.copy(part, index, kind, peer).start()

        def done():
            self.copy(part, index, kind, peer).wait_send()

        pl.when(where)(go)
        self.sent.append((where, done))

    def up(self, part, index, where):
        self.send(part, index, 0, jnp.minimum(self.me + self.nx, self.nz * self.nx - 1),
                  jnp.logical_and(where, self.z < self.nz - 1))

    def down(self, part, index, where):
        self.send(part, index, 1, jnp.maximum(self.me - self.nx, 0), jnp.logical_and(where, self.z > 0))

    def across(self, part, index, where):
        for k in range(1, self.nx):
            peer = self.z * self.nx + (self.x + k) % self.nx
            self.send(part, index, 1 + k, peer, where)

    def arrived(self, part, index, where):
        def go():
            self.copy(part, index, 0, self.me).wait_recv()
            if self.extra is not None:
                self.extra(part, index)

        pl.when(where)(go)

    def start(self):
        yes = self.z >= 0
        for part in range(self.direct, self.parts):
            self.across(part, self.me, yes)
        for part in range(self.parts):
            self.up(part, self.me, yes)
            self.down(part, self.me, yes)
            if part < self.direct:
                self.across(part, self.me, yes)

    def side(self):
        yes = self.z >= 0
        for part in range(self.direct, self.parts):
            for k in range(1, self.nx):
                index = self.z * self.nx + (self.x + k) % self.nx
                self.arrived(part, index, yes)
                self.up(part, index, yes)
                self.down(part, index, yes)

    def hop(self, s):
        below, above = self.z >= s, self.z + s < self.nz
        low = jnp.maximum(self.z - s, 0) * self.nx
        high = jnp.minimum(self.z + s, self.nz - 1) * self.nx
        ways = ((below, low, self.up), (above, high, self.down))
        for part in range(self.direct):
            for where, base, onward in ways:
                index = base + self.x
                self.arrived(part, index, where)
                onward(part, index, where)
                self.across(part, index, where)
        for part in range(self.direct, self.parts):
            for k in range(self.nx):
                for where, base, onward in ways:
                    index = base + (self.x + k) % self.nx
                    self.arrived(part, index, where)
                    onward(part, index, where)

    def last(self):
        yes = self.z >= 0
        for part in range(self.direct):
            for z in range(self.nz):
                for k in range(1, self.nx):
                    self.arrived(part, z * self.nx + (self.x + k) % self.nx, yes)

    def drain(self):
        for where, done in self.sent:
            pl.when(where)(done)

    def whole(self):
        self.start()
        self.side()
        for s in range(1, self.nz):
            self.hop(s)
        self.last()


def kernel(
    nfs, ntp, nz, nx, total_tokens, entries,
    x_in, cv_in, cq_in, mv_in, mq_in, fv_in, fq_in, v1_in, v2_in, q1_in, q2_in,
    step_v, step_q, new_v, new_q, copy_v, copy_q, v1, v2, q1, q2,
    xs, cv, cq, ct, gh, gl, fac, part, landed, dirs, sums, cop, mv, mq, m1v, m2v, m1q, m2q,
    load_sem, x_sem, fsend, frecv, sib_send, sib_recv, dsend, drecv, csend, crecv, rs_sem, sum_sem,
):
    me, tp = lax.axis_index("fs"), lax.axis_index("tp")
    core, sibling = tp % 2, tp + 1 - 2 * (tp % 2)
    blocks, tokens, width = xs.shape
    rows, rank = fv_in.shape
    wv, wq = cv.shape[1], cq.shape[1]
    rk = v1_in.shape[0]
    fparts, fhalf = fac.shape[2], fac.shape[3]
    dparts, dhalf = dirs.shape[1], dirs.shape[2]
    cparts, chalf = cop.shape[1], cop.shape[2]

    loads = []

    def load(src, dst):
        copy = pltpu.make_async_copy(src, dst, load_sem.at[len(loads)])
        copy.start()
        loads.append(copy)

    for p in range(fparts):
        load(fv_in.at[pl.ds(p * fhalf, fhalf)], fac.at[0, me, p])
        load(fq_in.at[pl.ds(p * fhalf, fhalf)], fac.at[1, me, p])
    nfac = len(loads)
    load(cv_in, cv)
    load(cq_in, cq)
    xcopies = []
    for b in range(blocks):
        copy = pltpu.make_async_copy(x_in.at[:, pl.ds(b * width, width)], xs.at[b], x_sem.at[b])
        copy.start()
        xcopies.append(copy)
    for src, dst in ((v1_in, m1v), (v2_in, m2v), (q1_in, m1q), (q2_in, m2q), (mv_in, mv), (mq_in, mq)):
        load(src, dst)

    barrier = pltpu.get_barrier_semaphore()

    def greet_fs(k, _):
        pl.semaphore_signal(barrier, inc=1, device_id={"fs": (me + k) % nfs}, device_id_type=MESH)
        return 0

    def greet_tp(k, _):
        pl.semaphore_signal(barrier, inc=1, device_id={"tp": (tp + k) % ntp}, device_id_type=MESH)
        return 0

    lax.fori_loop(1, nfs, greet_fs, 0)
    lax.fori_loop(1, ntp, greet_tp, 0)
    for copy in loads[:nfac]:
        copy.wait()
    pl.semaphore_wait(barrier, nfs + ntp - 2)

    def to_sibling(p, index):
        return pltpu.make_async_remote_copy(
            src_ref=fac.at[core, index, p],
            dst_ref=fac.at[core, index, p],
            send_sem=sib_send.at[p, index],
            recv_sem=sib_recv.at[p, index],
            device_id={"tp": sibling},
            device_id_type=MESH,
        )

    factors = Gather(
        lambda index, p: fac.at[core, index, p], fparts, nz, nx, me, fsend, frecv,
        extra=lambda p, index: to_sibling(p, index).start(),
    )
    factors.start()

    loads[nfac].wait()
    loads[nfac + 1].wait()
    ct[0:wv, :] = cv[...].T
    ct[wv : wv + wq, :] = cq[...].T
    inverse = 1.0 / total_tokens

    def grad_block(b):
        xcopies[b].wait()
        g = split_dot(ct[...], xs[b]) * inverse
        high = g.astype(BF16)
        gh[b] = high
        gl[b] = (g - high.astype(F32)).astype(BF16)

    todo = [factors.side] + [functools.partial(factors.hop, s) for s in range(1, nz)]
    for b in range(blocks):
        grad_block(b)
        if b < len(todo):
            todo[b]()
    for work in todo[blocks:]:
        work()
    factors.last()
    for p in range(fparts):
        for k in range(1, nfs):
            index = (me + k) % nfs
            pltpu.make_async_remote_copy(
                src_ref=fac.at[1 - core, index, p],
                dst_ref=fac.at[1 - core, index, p],
                send_sem=sib_send.at[p, index],
                recv_sem=sib_recv.at[p, index],
                device_id={"tp": sibling},
                device_id_type=MESH,
            ).wait_recv()

    all_v = fac[0].reshape(blocks, width, rank)
    all_q = fac[1].reshape(blocks, width, rank)
    acc_v = jnp.zeros((wv, rank), F32)
    acc_q = jnp.zeros((wq, rank), F32)
    for b in range(blocks):
        for g in (gl, gh):
            acc_v += split_dot(g[b, 0:wv, :], all_v[b])
            acc_q += split_dot(g[b, wv : wv + wq, :], all_q[b])
    part[:, :, 0:wv] = acc_v.T.reshape(nfs, rk, wv)
    part[:, :, wv : wv + wq] = acc_q.T.reshape(nfs, rk, wq)

    for k in range(1, nfs):
        peer = (me + k) % nfs
        pltpu.make_async_remote_copy(
            src_ref=part.at[peer],
            dst_ref=landed.at[k - 1],
            send_sem=rs_sem.at[0],
            recv_sem=rs_sem.at[1],
            device_id={"fs": peer},
            device_id_type=MESH,
        ).start()
    for copy in loads[nfac + 2 :]:
        copy.wait()
    everything = pltpu.make_async_remote_copy(
        src_ref=landed,
        dst_ref=landed,
        send_sem=rs_sem.at[0],
        recv_sem=rs_sem.at[1],
        device_id={"fs": me},
        device_id_type=MESH,
    )
    everything.wait_recv()
    share = part[me]
    for k in range(nfs - 1):
        share = share + landed[k]

    for cols, first_ref, second_ref, first_out, second_out in (
        (slice(0, wv), m1v, m2v, v1, v2),
        (slice(wv, wv + wq), m1q, m2q, q1, q2),
    ):
        projected = share[:, cols]
        first_new = BETA_ONE * first_ref[...] + (1.0 - BETA_ONE) * projected
        second_new = BETA_TWO * second_ref[...] + (1.0 - BETA_TWO) * projected * projected
        first_out[...] = first_new
        second_out[...] = second_new
        direction = first_new / (jnp.sqrt(second_new) + DENOM_EPS)
        dirs[me, :, :, cols] = direction.reshape(dparts, dhalf, direction.shape[1])

    directions = Gather(lambda index, p: dirs.at[index, p], dparts, nz, nx, me, dsend, drecv)
    directions.start()
    directions.side()
    for s in range(1, nz):
        directions.hop(s)
    directions.last()

    full = dirs[...].reshape(rank, wv + wq)
    sums[ntp - 1] = jnp.full(sums.shape[1:], jnp.sum(full * full), F32)

    def tell(k, _):
        pltpu.make_async_remote_copy(
            src_ref=sums.at[ntp - 1],
            dst_ref=sums.at[ntp - 1 - k],
            send_sem=sum_sem.at[0],
            recv_sem=sum_sem.at[1],
            device_id={"tp": (tp + k) % ntp},
            device_id_type=MESH,
        ).start()
        return 0

    lax.fori_loop(1, ntp, tell, 0)
    high = full.astype(BF16)
    low = (full - high.astype(F32)).astype(BF16)
    own_v = fac[0, me].reshape(rows, rank)
    own_q = fac[1, me].reshape(rows, rank)
    raw_v = split_dot(own_v, low[:, 0:wv]) + split_dot(own_v, high[:, 0:wv])
    raw_q = split_dot(own_q, low[:, wv:]) + split_dot(own_q, high[:, wv:])

    told = pltpu.make_async_remote_copy(
        src_ref=sums.at[pl.ds(0, ntp - 1)],
        dst_ref=sums.at[pl.ds(0, ntp - 1)],
        send_sem=sum_sem.at[0],
        recv_sem=sum_sem.at[1],
        device_id={"fs": me},
        device_id_type=MESH,
    )
    told.wait_recv()
    square_sum = jnp.sum(sums[...], axis=0)[0:1, 0:1]
    scale = 1.0 / jnp.sqrt(square_sum / entries + NORM_EPS)
    sv = raw_v * scale
    sq = raw_q * scale
    nv = mv[...] - STEP_SIZE * sv
    nq = mq[...] - STEP_SIZE * sq
    step_v[...] = sv
    step_q[...] = sq
    new_v[...] = nv
    new_q[...] = nq
    cop[me, :, :, 0:wv] = nv.astype(BF16).reshape(cparts, chalf, wv)
    cop[me, :, :, wv : wv + wq] = nq.astype(BF16).reshape(cparts, chalf, wq)
    copies = Gather(lambda index, p: cop.at[index, p], cparts, nz, nx, me, csend, crecv)
    copies.whole()
    copy_v[...] = cop[:, :, :, 0:wv].reshape(nfs * rows, wv)
    copy_q[...] = cop[:, :, :, wv : wv + wq].reshape(nfs * rows, wq)

    factors.drain()
    for p in range(fparts):
        for k in range(1, nfs):
            to_sibling(p, (me + k) % nfs).wait_send()
    everything.wait_send()
    told.wait_send()
    directions.drain()
    copies.drain()


def hand_over(*refs):
    sem, count = refs[-1], len(refs) // 2
    copies = [pltpu.make_async_copy(refs[i], refs[count + i], sem.at[i]) for i in range(count)]
    for copy in copies:
        copy.start()
    for copy in copies:
        copy.wait()


def grid_of(n):
    nx = 1
    for d in range(1, n + 1):
        if n % d == 0 and d * d <= n:
            nx = d
    return n // nx, nx


def solution(mesh):
    nfs, ntp = mesh.shape["fs"], mesh.shape["tp"]
    nz, nx = grid_of(nfs)

    def step(x, cv, cq, mv, mq, fv, fq, v1, v2, q1, q2):
        tokens, depth = x.shape
        wv, wq = cv.shape[1], cq.shape[1]
        rows, rank = fv.shape
        rk = v1.shape[0]
        w = wv + wq
        blocks = 4
        width = depth // blocks
        four = lambda size, tile: 4 if size % (4 * tile) == 0 else 1
        fparts, dparts, cparts = four(rows, 16), 1, four(rows, 16)
        kinds = 1 + nx
        dma = pltpu.SemaphoreType.DMA
        like = lambda shape, dtype: jax.ShapeDtypeStruct(shape, dtype)
        outs = pl.pallas_call(
            functools.partial(
                kernel, nfs, ntp, nz, nx, float(tokens * nfs), float(rank * w * ntp)
            ),
            out_shape=(
                like((rows, wv), F32), like((rows, wq), F32),
                like((rows, wv), F32), like((rows, wq), F32),
                like((depth, wv), BF16), like((depth, wq), BF16),
                like((rk, wv), F32), like((rk, wv), F32),
                like((rk, wq), F32), like((rk, wq), F32),
            ),
            in_specs=[pl.BlockSpec(memory_space=pl.ANY)] * 11,
            out_specs=tuple([pl.BlockSpec(memory_space=pltpu.VMEM)] * 10),
            scratch_shapes=[
                pltpu.VMEM((blocks, tokens, width), BF16),
                pltpu.VMEM((tokens, wv), BF16),
                pltpu.VMEM((tokens, wq), BF16),
                pltpu.VMEM((w, tokens), BF16),
                pltpu.VMEM((blocks, w, width), BF16),
                pltpu.VMEM((blocks, w, width), BF16),
                pltpu.VMEM((2, nfs, fparts, rows // fparts, rank), BF16),
                pltpu.VMEM((nfs, rk, w), F32),
                pltpu.VMEM((nfs - 1, rk, w), F32),
                pltpu.VMEM((nfs, dparts, rk // dparts, w), F32),
                pltpu.VMEM((ntp, 8, 128), F32),
                pltpu.VMEM((nfs, cparts, rows // cparts, w), BF16),
                pltpu.VMEM((rows, wv), F32),
                pltpu.VMEM((rows, wq), F32),
                pltpu.VMEM((rk, wv), F32),
                pltpu.VMEM((rk, wv), F32),
                pltpu.VMEM((rk, wq), F32),
                pltpu.VMEM((rk, wq), F32),
                dma((2 * fparts + 8,)),
                dma((blocks,)),
                dma((fparts, nfs, kinds)),
                dma((fparts, nfs)),
                dma((fparts, nfs)),
                dma((fparts, nfs)),
                dma((dparts, nfs, kinds)),
                dma((dparts, nfs)),
                dma((cparts, nfs, kinds)),
                dma((cparts, nfs)),
                dma((2,)),
                dma((2,)),
            ],
            compiler_params=pltpu.CompilerParams(
                collective_id=0, has_side_effects=True, vmem_limit_bytes=36 * 1024 * 1024
            ),
            name="moment_step",
        )(x, cv, cq, mv, mq, fv, fq, v1, v2, q1, q2)
        return pl.pallas_call(
            hand_over,
            out_shape=tuple(like(o.shape, o.dtype) for o in outs),
            in_specs=[pl.BlockSpec(memory_space=pltpu.VMEM)] * len(outs),
            out_specs=tuple([pl.BlockSpec(memory_space=pl.ANY)] * len(outs)),
            scratch_shapes=[dma((len(outs),))],
            compiler_params=pltpu.CompilerParams(vmem_limit_bytes=8 * 1024 * 1024),
            name="hand_over",
        )(*outs)

    tall, both = P("fs", None), P("fs", "tp")
    return jax.shard_map(
        step,
        mesh=mesh,
        in_specs=(tall, both, both, both, both, tall, tall, both, both, both, both),
        out_specs=(both, both, both, both, P(None, "tp"), P(None, "tp"), both, both, both, both),
        check_vma=False,
    )
```

```python
import functools

import jax
import jax.numpy as jnp
from jax import lax
from jax.experimental import pallas as pl
from jax.experimental.pallas import tpu as pltpu
from jax.sharding import PartitionSpec as P

BETA_ONE = 0.9
BETA_TWO = 0.95
DENOM_EPS = 1e-08
NORM_EPS = 1e-06
STEP_SIZE = 0.05

MESH = pl.DeviceIdType.MESH
F32 = jnp.float32
BF16 = jnp.bfloat16


def split_dot(lhs, rhs):
    return jnp.dot(lhs, rhs, preferred_element_type=F32)


class Gather:
    def __init__(self, slot, parts, nz, nx, me, send_sem, recv_sem, extra=None):
        self.slot, self.parts, self.nz, self.nx = slot, parts, nz, nx
        self.me, self.z, self.x = me, me // nx, me % nx
        self.send_sem, self.recv_sem, self.extra = send_sem, recv_sem, extra
        self.sent = []
        self.direct = max(parts - 1, 1)

    def copy(self, part, index, kind, peer):
        ref = self.slot(index, part)
        return pltpu.make_async_remote_copy(
            src_ref=ref,
            dst_ref=ref,
            send_sem=self.send_sem.at[part, index, kind],
            recv_sem=self.recv_sem.at[part, index],
            device_id={"fs": peer},
            device_id_type=MESH,
        )

    def send(self, part, index, kind, peer, where):
        def go():
            self.copy(part, index, kind, peer).start()

        def done():
            self.copy(part, index, kind, peer).wait_send()

        pl.when(where)(go)
        self.sent.append((where, done))

    def up(self, part, index, where):
        self.send(part, index, 0, jnp.minimum(self.me + self.nx, self.nz * self.nx - 1),
                  jnp.logical_and(where, self.z < self.nz - 1))

    def down(self, part, index, where):
        self.send(part, index, 1, jnp.maximum(self.me - self.nx, 0), jnp.logical_and(where, self.z > 0))

    def across(self, part, index, where):
        for k in range(1, self.nx):
            peer = self.z * self.nx + (self.x + k) % self.nx
            self.send(part, index, 1 + k, peer, where)

    def arrived(self, part, index, where):
        def go():
            self.copy(part, index, 0, self.me).wait_recv()
            if self.extra is not None:
                self.extra(part, index)

        pl.when(where)(go)

    def start(self):
        yes = self.z >= 0
        for part in range(self.direct, self.parts):
            self.across(part, self.me, yes)
        for part in range(self.parts):
            self.up(part, self.me, yes)
            self.down(part, self.me, yes)
            if part < self.direct:
                self.across(part, self.me, yes)

    def side(self):
        yes = self.z >= 0
        for part in range(self.direct, self.parts):
            for k in range(1, self.nx):
                index = self.z * self.nx + (self.x + k) % self.nx
                self.arrived(part, index, yes)
                self.up(part, index, yes)
                self.down(part, index, yes)

    def hop(self, s):
        below, above = self.z >= s, self.z + s < self.nz
        low = jnp.maximum(self.z - s, 0) * self.nx
        high = jnp.minimum(self.z + s, self.nz - 1) * self.nx
        ways = ((below, low, self.up), (above, high, self.down))
        for part in range(self.direct):
            for where, base, onward in ways:
                index = base + self.x
                self.arrived(part, index, where)
                onward(part, index, where)
                self.across(part, index, where)
        for part in range(self.direct, self.parts):
            for k in range(self.nx):
                for where, base, onward in ways:
                    index = base + (self.x + k) % self.nx
                    self.arrived(part, index, where)
                    onward(part, index, where)

    def last(self):
        yes = self.z >= 0
        for part in range(self.direct):
            for z in range(self.nz):
                for k in range(1, self.nx):
                    self.arrived(part, z * self.nx + (self.x + k) % self.nx, yes)

    def drain(self):
        for where, done in self.sent:
            pl.when(where)(done)

    def whole(self):
        self.start()
        self.side()
        for s in range(1, self.nz):
            self.hop(s)
        self.last()


def kernel(
    nfs, ntp, nz, nx, total_tokens, entries,
    x_in, cv_in, cq_in, mv_in, mq_in, fv_in, fq_in, v1_in, v2_in, q1_in, q2_in,
    step_v, step_q, new_v, new_q, copy_v, copy_q, v1, v2, q1, q2,
    xs, cv, cq, ct, gh, gl, fac, part, landed, dirs, sums, cop, mv, mq, m1v, m2v, m1q, m2q,
    load_sem, x_sem, fsend, frecv, sib_send, sib_recv, dsend, drecv, csend, crecv, rs_sem, sum_sem,
):
    me, tp = lax.axis_index("fs"), lax.axis_index("tp")
    core, sibling = tp % 2, tp + 1 - 2 * (tp % 2)
    blocks, tokens, width = xs.shape
    rows, rank = fv_in.shape
    wv, wq = cv.shape[1], cq.shape[1]
    rk = v1_in.shape[0]
    fparts, fhalf = fac.shape[2], fac.shape[3]
    dparts, dhalf = dirs.shape[1], dirs.shape[2]
    cparts, chalf = cop.shape[1], cop.shape[2]

    loads = []

    def load(src, dst):
        copy = pltpu.make_async_copy(src, dst, load_sem.at[len(loads)])
        copy.start()
        loads.append(copy)

    for p in range(fparts):
        load(fv_in.at[pl.ds(p * fhalf, fhalf)], fac.at[0, me, p])
        load(fq_in.at[pl.ds(p * fhalf, fhalf)], fac.at[1, me, p])
    nfac = len(loads)
    load(cv_in, cv)
    load(cq_in, cq)
    xcopies = []
    for b in range(blocks):
        copy = pltpu.make_async_copy(x_in.at[:, pl.ds(b * width, width)], xs.at[b], x_sem.at[b])
        copy.start()
        xcopies.append(copy)
    for src, dst in ((v1_in, m1v), (v2_in, m2v), (q1_in, m1q), (q2_in, m2q), (mv_in, mv), (mq_in, mq)):
        load(src, dst)

    barrier = pltpu.get_barrier_semaphore()

    def greet_fs(k, _):
        pl.semaphore_signal(barrier, inc=1, device_id={"fs": (me + k) % nfs}, device_id_type=MESH)
        return 0

    def greet_tp(k, _):
        pl.semaphore_signal(barrier, inc=1, device_id={"tp": (tp + k) % ntp}, device_id_type=MESH)
        return 0

    lax.fori_loop(1, nfs, greet_fs, 0)
    lax.fori_loop(1, ntp, greet_tp, 0)
    for copy in loads[:nfac]:
        copy.wait()
    pl.semaphore_wait(barrier, nfs + ntp - 2)

    def to_sibling(p, index):
        return pltpu.make_async_remote_copy(
            src_ref=fac.at[core, index, p],
            dst_ref=fac.at[core, index, p],
            send_sem=sib_send.at[p, index],
            recv_sem=sib_recv.at[p, index],
            device_id={"tp": sibling},
            device_id_type=MESH,
        )

    factors = Gather(
        lambda index, p: fac.at[core, index, p], fparts, nz, nx, me, fsend, frecv,
        extra=lambda p, index: to_sibling(p, index).start(),
    )
    factors.start()

    loads[nfac].wait()
    loads[nfac + 1].wait()
    ct[0:wv, :] = cv[...].T
    ct[wv : wv + wq, :] = cq[...].T
    inverse = 1.0 / total_tokens

    def grad_block(b):
        xcopies[b].wait()
        g = split_dot(ct[...], xs[b]) * inverse
        high = g.astype(BF16)
        gh[b] = high
        gl[b] = (g - high.astype(F32)).astype(BF16)

    todo = [factors.side] + [functools.partial(factors.hop, s) for s in range(1, nz)]
    for b in range(blocks):
        grad_block(b)
        if b < len(todo):
            todo[b]()
    for work in todo[blocks:]:
        work()
    factors.last()
    for p in range(fparts):
        for k in range(1, nfs):
            index = (me + k) % nfs
            pltpu.make_async_remote_copy(
                src_ref=fac.at[1 - core, index, p],
                dst_ref=fac.at[1 - core, index, p],
                send_sem=sib_send.at[p, index],
                recv_sem=sib_recv.at[p, index],
                device_id={"tp": sibling},
                device_id_type=MESH,
            ).wait_recv()

    all_v = fac[0].reshape(blocks, width, rank)
    all_q = fac[1].reshape(blocks, width, rank)
    acc_v = jnp.zeros((wv, rank), F32)
    acc_q = jnp.zeros((wq, rank), F32)
    for b in range(blocks):
        for g in (gl, gh):
            acc_v += split_dot(g[b, 0:wv, :], all_v[b])
            acc_q += split_dot(g[b, wv : wv + wq, :], all_q[b])
    part[:, :, 0:wv] = acc_v.T.reshape(nfs, rk, wv)
    part[:, :, wv : wv + wq] = acc_q.T.reshape(nfs, rk, wq)

    for k in range(1, nfs):
        peer = (me + k) % nfs
        pltpu.make_async_remote_copy(
            src_ref=part.at[peer],
            dst_ref=landed.at[k - 1],
            send_sem=rs_sem.at[0],
            recv_sem=rs_sem.at[1],
            device_id={"fs": peer},
            device_id_type=MESH,
        ).start()
    for copy in loads[nfac + 2 :]:
        copy.wait()
    everything = pltpu.make_async_remote_copy(
        src_ref=landed,
        dst_ref=landed,
        send_sem=rs_sem.at[0],
        recv_sem=rs_sem.at[1],
        device_id={"fs": me},
        device_id_type=MESH,
    )
    everything.wait_recv()
    share = part[me]
    for k in range(nfs - 1):
        share = share + landed[k]

    for cols, first_ref, second_ref, first_out, second_out in (
        (slice(0, wv), m1v, m2v, v1, v2),
        (slice(wv, wv + wq), m1q, m2q, q1, q2),
    ):
        projected = share[:, cols]
        first_new = BETA_ONE * first_ref[...] + (1.0 - BETA_ONE) * projected
        second_new = BETA_TWO * second_ref[...] + (1.0 - BETA_TWO) * projected * projected
        first_out[...] = first_new
        second_out[...] = second_new
        direction = first_new / (jnp.sqrt(second_new) + DENOM_EPS)
        dirs[me, :, :, cols] = direction.reshape(dparts, dhalf, direction.shape[1])

    directions = Gather(lambda index, p: dirs.at[index, p], dparts, nz, nx, me, dsend, drecv)
    directions.start()
    directions.side()
    for s in range(1, nz):
        directions.hop(s)
    directions.last()

    full = dirs[...].reshape(rank, wv + wq)
    sums[ntp - 1] = jnp.full(sums.shape[1:], jnp.sum(full * full), F32)

    def tell(k, _):
        pltpu.make_async_remote_copy(
            src_ref=sums.at[ntp - 1],
            dst_ref=sums.at[ntp - 1 - k],
            send_sem=sum_sem.at[0],
            recv_sem=sum_sem.at[1],
            device_id={"tp": (tp + k) % ntp},
            device_id_type=MESH,
        ).start()
        return 0

    lax.fori_loop(1, ntp, tell, 0)
    high = full.astype(BF16)
    low = (full - high.astype(F32)).astype(BF16)
    own_v = fac[0, me].reshape(rows, rank)
    own_q = fac[1, me].reshape(rows, rank)
    raw_v = split_dot(own_v, low[:, 0:wv]) + split_dot(own_v, high[:, 0:wv])
    raw_q = split_dot(own_q, low[:, wv:]) + split_dot(own_q, high[:, wv:])

    told = pltpu.make_async_remote_copy(
        src_ref=sums.at[pl.ds(0, ntp - 1)],
        dst_ref=sums.at[pl.ds(0, ntp - 1)],
        send_sem=sum_sem.at[0],
        recv_sem=sum_sem.at[1],
        device_id={"fs": me},
        device_id_type=MESH,
    )
    told.wait_recv()
    square_sum = jnp.sum(sums[...], axis=0)[0:1, 0:1]
    scale = 1.0 / jnp.sqrt(square_sum / entries + NORM_EPS)
    sv = raw_v * scale
    sq = raw_q * scale
    nv = mv[...] - STEP_SIZE * sv
    nq = mq[...] - STEP_SIZE * sq
    step_v[...] = sv
    step_q[...] = sq
    new_v[...] = nv
    new_q[...] = nq
    cop[me, :, :, 0:wv] = nv.astype(BF16).reshape(cparts, chalf, wv)
    cop[me, :, :, wv : wv + wq] = nq.astype(BF16).reshape(cparts, chalf, wq)
    copies = Gather(lambda index, p: cop.at[index, p], cparts, nz, nx, me, csend, crecv)
    copies.whole()
    copy_v[...] = cop[:, :, :, 0:wv].reshape(nfs * rows, wv)
    copy_q[...] = cop[:, :, :, wv : wv + wq].reshape(nfs * rows, wq)

    factors.drain()
    for p in range(fparts):
        for k in range(1, nfs):
            to_sibling(p, (me + k) % nfs).wait_send()
    everything.wait_send()
    told.wait_send()
    directions.drain()
    copies.drain()


def hand_over(*refs):
    sem, count = refs[-1], len(refs) // 3
    source, result, held = refs[:count], refs[count : 2 * count], refs[2 * count : 3 * count]
    takes = [pltpu.make_async_copy(source[i], held[i], sem.at[0, i]) for i in range(count)]
    gives = [pltpu.make_async_copy(held[i], result[i], sem.at[1, i]) for i in range(count)]
    for take in takes:
        take.start()
    for take, give in zip(takes, gives):
        take.wait()
        give.start()
    for give in gives:
        give.wait()


def grid_of(n):
    nx = 1
    for d in range(1, n + 1):
        if n % d == 0 and d * d <= n:
            nx = d
    return n // nx, nx


def solution(mesh):
    nfs, ntp = mesh.shape["fs"], mesh.shape["tp"]
    nz, nx = grid_of(nfs)

    def step(x, cv, cq, mv, mq, fv, fq, v1, v2, q1, q2):
        tokens, depth = x.shape
        wv, wq = cv.shape[1], cq.shape[1]
        rows, rank = fv.shape
        rk = v1.shape[0]
        w = wv + wq
        blocks = 4
        width = depth // blocks
        four = lambda size, tile: 4 if size % (4 * tile) == 0 else 1
        fparts, dparts, cparts = four(rows, 16), 1, four(rows, 16)
        kinds = 1 + nx
        dma = pltpu.SemaphoreType.DMA
        like = lambda shape, dtype: jax.ShapeDtypeStruct(shape, dtype)
        outs = pl.pallas_call(
            functools.partial(
                kernel, nfs, ntp, nz, nx, float(tokens * nfs), float(rank * w * ntp)
            ),
            out_shape=(
                like((rows, wv), F32), like((rows, wq), F32),
                like((rows, wv), F32), like((rows, wq), F32),
                like((depth, wv), BF16), like((depth, wq), BF16),
                like((rk, wv), F32), like((rk, wv), F32),
                like((rk, wq), F32), like((rk, wq), F32),
            ),
            in_specs=[pl.BlockSpec(memory_space=pltpu.HBM)] * 11,
            out_specs=tuple([pl.BlockSpec(memory_space=pltpu.VMEM)] * 10),
            scratch_shapes=[
                pltpu.VMEM((blocks, tokens, width), BF16),
                pltpu.VMEM((tokens, wv), BF16),
                pltpu.VMEM((tokens, wq), BF16),
                pltpu.VMEM((w, tokens), BF16),
                pltpu.VMEM((blocks, w, width), BF16),
                pltpu.VMEM((blocks, w, width), BF16),
                pltpu.VMEM((2, nfs, fparts, rows // fparts, rank), BF16),
                pltpu.VMEM((nfs, rk, w), F32),
                pltpu.VMEM((nfs - 1, rk, w), F32),
                pltpu.VMEM((nfs, dparts, rk // dparts, w), F32),
                pltpu.VMEM((ntp, 8, 128), F32),
                pltpu.VMEM((nfs, cparts, rows // cparts, w), BF16),
                pltpu.VMEM((rows, wv), F32),
                pltpu.VMEM((rows, wq), F32),
                pltpu.VMEM((rk, wv), F32),
                pltpu.VMEM((rk, wv), F32),
                pltpu.VMEM((rk, wq), F32),
                pltpu.VMEM((rk, wq), F32),
                dma((2 * fparts + 8,)),
                dma((blocks,)),
                dma((fparts, nfs, kinds)),
                dma((fparts, nfs)),
                dma((fparts, nfs)),
                dma((fparts, nfs)),
                dma((dparts, nfs, kinds)),
                dma((dparts, nfs)),
                dma((cparts, nfs, kinds)),
                dma((cparts, nfs)),
                dma((2,)),
                dma((2,)),
            ],
            compiler_params=pltpu.CompilerParams(
                collective_id=0, has_side_effects=True, vmem_limit_bytes=60 * 1024 * 1024
            ),
            name="moment_step",
        )(x, cv, cq, mv, mq, fv, fq, v1, v2, q1, q2)
        return pl.pallas_call(
            hand_over,
            out_shape=tuple(like(o.shape, o.dtype) for o in outs),
            in_specs=[pl.BlockSpec(memory_space=pl.ANY)] * len(outs),
            out_specs=tuple([pl.BlockSpec(memory_space=pl.ANY)] * len(outs)),
            scratch_shapes=[pltpu.VMEM(o.shape, o.dtype) for o in outs] + [dma((2, len(outs)))],
            compiler_params=pltpu.CompilerParams(vmem_limit_bytes=60 * 1024 * 1024),
            name="hand_over",
        )(*outs)

    tall, both = P("fs", None), P("fs", "tp")
    return jax.shard_map(
        step,
        mesh=mesh,
        in_specs=(tall, both, both, both, both, tall, tall, both, both, both, both),
        out_specs=(both, both, both, both, P(None, "tp"), P(None, "tp"), both, both, both, both),
        check_vma=False,
    )
```
